32 devices in a mesh: ep: 8 (over z, x), tp: 4 (over y, core).
Axes of the slice: x: 2, y: 2, z: 4, core: 2. Of those that a mesh axis runs over, the one named last changes fastest.
Arguments:
- residual: bfloat16 [512, 4096], P('ep', 'tp'), may hold values from -64 to 64
- routes: int32 [512, 2], P('ep'), may hold values from 0 to 7, all different within a row; in each aligned block of 64 rows (0 to 63, 64 to 127, ...) at most 32 rows name the same one
- route_weights: float32 [512, 2], P('ep'), may hold values from 0.2 to 1
- state_prev: float32 [512, 2, 64, 64], P('ep', None, 'tp'), may hold values from -6 to 6
- mix_gain: float32 [4096], replicated, may hold values from 0.1 to 1.9
- ffn_gain: float32 [4096], replicated, may hold values from 0.1 to 1.9
- w_in: bfloat16 [4096, 1024], P(None, 'tp'), may hold values from -0.09375 to 0.09375
- decay_rate: float32 [64, 64], P('tp'), may hold values from 0.5 to 8
- rotation: float32 [64, 64], P('tp'), may hold values from 0 to 200
- log_step: float32 [64], P('tp'), may hold values from -3.9 to -1.2
- in_re: float32 [64, 64, 16], P('tp'), may hold values from -1 to 1
- in_im: float32 [64, 64, 16], P('tp'), may hold values from -1 to 1
- read_re: float32 [64, 16, 64], P('tp'), may hold values from -0.5 to 0.5
- read_im: float32 [64, 16, 64], P('tp'), may hold values from -0.5 to 0.5
- skip_gain: float32 [64, 16], P('tp'), may hold values from -4 to 4
- w_glu: bfloat16 [1024, 1024], P(None, 'tp'), may hold values from -0.1875 to 0.1875
- w_out: bfloat16 [1024, 4096], P('tp'), may hold values from -0.1875 to 0.1875
- w_gate: bfloat16 [8, 4096, 5632], P('ep', None, 'tp'), may hold values from -0.09375 to 0.09375
- w_up: bfloat16 [8, 4096, 5632], P('ep', None, 'tp'), may hold values from -0.09375 to 0.09375
- w_down: bfloat16 [8, 5632, 4096], P('ep', 'tp'), may hold values from -0.078125 to 0.078125
Outputs:
- layer_out: bfloat16 [512, 4096], P('ep', 'tp')
- state_next: float32 [512, 2, 64, 64], P('ep', None, 'tp')
The draws below stay inside these ranges and needn't reach their ends.
Inputs may be any that keep to these rules, and one draw needn't show every extreme that they name: `routes`: each row names 2 different experts. In each aligned block of 64 rows (the rows of one index of ep) no expert is named more than 32 times, a bound that some block reaches.
All inputs are finite; a program needn't handle non-finite values.
Results may differ from the reference program's by a relative error of at most 0.012.
Values may be sent and summed in bfloat16 or wider, within the bound.
A program may use at most 128 MiB of HBM per device.

```python
import math
import jax
import jax.numpy as jnp
import numpy as np
from jax import lax

D = 4096
CHAN = 1024
GROUP_CH = 16
GROUPS = 64
STATE = 64
FF_EXP = 5632
TOPK = 2
SEQ_GRP = 64
SEQS = 512
EXPERTS = 8
CAP = 32
N_EP = 8
N_TP = 4


def draw_residual(key, part):
    first_key, second_key = jax.random.split(jax.random.fold_in(key, 11))
    column_pos = jnp.arange(D, dtype=jnp.float32) / D
    row_scale = jnp.exp(math.log(10.0) * (jax.random.uniform(second_key, (SEQS, 1), jnp.float32) - 0.5))
    base_values = jnp.clip(jax.random.normal(first_key, (SEQS, D), jnp.float32), -6.0, 6.0)
    column_scale = jnp.exp(math.log(10.0) * (column_pos - 0.5))
    return (base_values * column_scale[None, :] * row_scale).astype(jnp.bfloat16)


def shard_levels(rng, dims, cuts, low, largest):
    def one(dim, shards_of):
        heights = jax.random.uniform(jax.random.fold_in(jax.random.fold_in(rng, 6), dim), (shards_of,), jnp.float32, low / len(cuts), largest / len(cuts))
        return jnp.repeat(jnp.exp(heights), dims[dim] // shards_of).reshape((-1,) + (1,) * (len(dims) - dim - 1))

    factor_of = one(*cuts[0])
    for cut in cuts[1:]:
        factor_of = factor_of * one(*cut)
    return factor_of


def deal_out(own_key, own, number, rows, number_of, top, limit, lean):
    sequence = jax.random.permutation(own_key, number_of)
    packed, usual = portions_of(number_of, rows * top, limit, lean, True), portions_of(number_of, rows * top, limit, lean, False)
    places = jnp.arange(number_of)

    def named(sizes, turn):
        used = int((sizes > 0).sum())
        fixed = max(1, used // 4)
        moved = fixed + (places - fixed + turn * (used - fixed)) % max(1, number_of - fixed)
        return jnp.zeros((number_of,), jnp.int32).at[sequence[jnp.where(places < fixed, places, moved)]].set(jnp.asarray(sizes, jnp.int32))

    sizes = jnp.where(number % 4 == 0, named(packed, number // 4), named(usual, number - number // 4 - 1))
    mixed = jax.random.permutation(jax.random.fold_in(own, 3), number_of)
    giver, taker = mixed[0:number_of // 2 * 2:2], mixed[1:number_of // 2 * 2:2]
    room = jnp.minimum(sizes[giver] - 1, limit - sizes[taker]) // 2
    room = jnp.where((giver == sequence[0]) | (taker == sequence[0]) | (sizes[taker] == 0), 0, jnp.maximum(room, 0))
    moved = jax.random.randint(jax.random.fold_in(own, 4), (number_of // 2,), 0, 1 << 20) % (room + 1)
    sizes = sizes.at[giver].add(-moved).at[taker].add(moved)
    items = jnp.searchsorted(jnp.cumsum(sizes), jnp.arange(rows * top), side="right").astype(jnp.int32)
    listing = items.reshape(top, rows).T
    listing = listing[jax.random.permutation(jax.random.fold_in(own, 1), rows)]
    turn = jax.random.randint(jax.random.fold_in(own, 2), (rows, 1), 0, top)
    return jnp.take_along_axis(listing, (jnp.arange(top)[None, :] + turn) % top, axis=1)


def portions_of(amount, total, reach, lean, full):
    portions = [(1 << 20) // math.isqrt(rank ** lean) + 1 for rank in range(1, amount + 1)]
    largest = reach if full else min(reach, max(-(-total // amount), total * portions[0] // sum(portions)))
    least = 1 if total - largest >= amount - 1 else 0
    holding, surplus = [largest] + [least] * (amount - 1), total - largest - least * (amount - 1)
    while surplus > 0:
        movable = [i for i in range(1, amount) if holding[i] < largest] or [i for i in range(1, amount) if holding[i] < reach]
        mass, left = sum([portions[i] for i in movable]), surplus
        for i in movable:
            addition = min(reach - holding[i], max(1, left * portions[i] // mass), surplus)
            holding[i] = holding[i] + addition
            surplus = surplus - addition
    return np.array(holding)


def noise(rng, dims, deviation, bound, shards=(), held_as=jnp.bfloat16):
    factor_of = shard_levels(rng, dims, shards, -0.22, 0.18) if shards else 1.0
    array = jax.random.normal(rng, dims, jnp.float32) * deviation * factor_of
    return jnp.minimum(jnp.maximum(array, -bound), bound).astype(held_as)


def setup_inputs(seed: int = 0) -> dict:
    keys = jax.random.split(jax.random.key(seed), 21)
    residual = draw_residual(jax.random.fold_in(keys[20], 71), 0)
    routes_keys = jax.random.split(jax.random.fold_in(keys[1], 1), SEQS // SEQ_GRP)
    routes_turns = jax.random.permutation(jax.random.fold_in(keys[1], 3), SEQS // SEQ_GRP)
    routes = jax.vmap(lambda own, number: deal_out(jax.random.fold_in(keys[1], 2), own, number, SEQ_GRP, EXPERTS, TOPK, CAP, 1))(routes_keys, routes_turns).reshape((SEQS, TOPK))
    route_weights = jnp.clip(0.2 + 0.8 * jax.random.uniform(keys[2], (SEQS, TOPK), jnp.float32) ** shard_levels(keys[2], (SEQS, TOPK), ((0, 8),), -0.2, 0.2), 0.2, 1.0)
    state_prev = noise(keys[3], (SEQS, 2, GROUPS, STATE), 1.0, 6.0, ((0, 8), (2, 4)), jnp.float32)
    mix_gain = jnp.clip(1.0 + 0.18 * jax.random.normal(keys[4], (D,), jnp.float32), 0.1, 1.9)
    ffn_gain = jnp.clip(1.0 + 0.18 * jax.random.normal(keys[5], (D,), jnp.float32), 0.1, 1.9)
    w_in = noise(keys[6], (D, CHAN), D ** -0.5, 0.09375, ((1, 4),))
    decay_rate = jnp.clip(jnp.exp(math.log(8.0) - 2.7725887 * jax.random.uniform(keys[7], (GROUPS, STATE), jnp.float32) ** shard_levels(keys[7], (GROUPS, STATE), ((0, 4),), -0.2, 0.2)), 0.5, 8.0)
    rotation = jnp.clip(200.0 * jax.random.uniform(keys[8], (GROUPS, STATE), jnp.float32) ** shard_levels(keys[8], (GROUPS, STATE), ((0, 4),), -0.2, 0.2), 0.0, 200.0)
    log_step = jnp.clip(-3.9 + 2.7 * jax.random.uniform(keys[9], (GROUPS,), jnp.float32) ** shard_levels(keys[9], (GROUPS,), ((0, 4),), -0.2, 0.2), -3.9, -1.2)
    in_re = noise(keys[10], (GROUPS, STATE, GROUP_CH), (2 * GROUP_CH) ** -0.5, 1.0, ((0, 4),), jnp.float32)
    in_im = noise(keys[11], (GROUPS, STATE, GROUP_CH), (2 * GROUP_CH) ** -0.5, 1.0, ((0, 4),), jnp.float32)
    read_re = noise(keys[12], (GROUPS, GROUP_CH, STATE), (2 * STATE) ** -0.5, 0.5, ((0, 4),), jnp.float32)
    read_im = noise(keys[13], (GROUPS, GROUP_CH, STATE), (2 * STATE) ** -0.5, 0.5, ((0, 4),), jnp.float32)
    skip_gain = noise(keys[14], (GROUPS, GROUP_CH), 1.0, 4.0, ((0, 4),), jnp.float32)
    w_glu = noise(keys[15], (CHAN, CHAN), CHAN ** -0.5, 0.1875, ((1, 4),))
    w_out = noise(keys[16], (CHAN, D), CHAN ** -0.5, 0.1875, ((0, 4),))
    w_gate = noise(keys[17], (EXPERTS, D, FF_EXP), D ** -0.5, 0.09375, ((0, 8), (2, 4)))
    w_up = noise(keys[18], (EXPERTS, D, FF_EXP), D ** -0.5, 0.09375, ((0, 8), (2, 4)))
    w_down = noise(keys[19], (EXPERTS, FF_EXP, D), FF_EXP ** -0.5, 0.078125, ((0, 8), (1, 4)))
    return dict(residual=residual, routes=routes, route_weights=route_weights, state_prev=state_prev, mix_gain=mix_gain, ffn_gain=ffn_gain, w_in=w_in, decay_rate=decay_rate, rotation=rotation, log_step=log_step, in_re=in_re, in_im=in_im, read_re=read_re, read_im=read_im, skip_gain=skip_gain, w_glu=w_glu, w_out=w_out, w_gate=w_gate, w_up=w_up, w_down=w_down)


epsilon = 1e-06
highest = lax.Precision.HIGHEST

def inverse_rms(values):
    return lax.rsqrt(lax.optimization_barrier(jnp.mean(values * values, axis=-1, keepdims=True)) + epsilon)

def state_mixer(u_in, state_prev, decay_rate, rotation, log_step, in_re, in_im, read_re, read_im, skip_gain):
    batch_rows = u_in.shape[0]
    groups = decay_rate.shape[0]
    grouped = u_in.astype(jnp.float32).reshape(batch_rows, groups, GROUP_CH)
    step_size = jnp.exp(log_step)[:, None]
    real_part = -decay_rate
    magnitude = jnp.exp(real_part * step_size)
    decay_re = magnitude * jnp.cos(rotation * step_size)
    decay_im = magnitude * jnp.sin(rotation * step_size)
    denominator = real_part * real_part + rotation * rotation
    lift_re = ((decay_re - 1.0) * real_part + decay_im * rotation) / denominator
    lift_im = (decay_im * real_part - (decay_re - 1.0) * rotation) / denominator
    map_re = lift_re[..., None] * in_re - lift_im[..., None] * in_im
    map_im = lift_re[..., None] * in_im + lift_im[..., None] * in_re
    drive_re = jnp.einsum('gph,bgh->bgp', map_re, grouped, precision=highest)
    drive_im = jnp.einsum('gph,bgh->bgp', map_im, grouped, precision=highest)
    old_re = state_prev[:, 0]
    old_im = state_prev[:, 1]
    new_re = decay_re * old_re - decay_im * old_im + drive_re
    new_im = decay_re * old_im + decay_im * old_re + drive_im
    output = jnp.einsum('ghp,bgp->bgh', read_re, new_re, precision=highest) - jnp.einsum('ghp,bgp->bgh', read_im, new_im, precision=highest) + skip_gain * grouped
    return (jax.nn.gelu(output.reshape(batch_rows, -1)), jnp.stack([new_re, new_im], axis=1))

def reference(residual, routes, route_weights, state_prev, mix_gain, ffn_gain, w_in, decay_rate, rotation, log_step, in_re, in_im, read_re, read_im, skip_gain, w_glu, w_out, w_gate, w_up, w_down):
    source = residual.astype(jnp.float32)
    normed_mix = (source * inverse_rms(source) * mix_gain).astype(jnp.bfloat16)
    u_in = jnp.dot(normed_mix, w_in, preferred_element_type=jnp.float32).astype(jnp.bfloat16)
    mixer_act, state_next = state_mixer(u_in, state_prev, decay_rate, rotation, log_step, in_re, in_im, read_re, read_im, skip_gain)
    mixer_bf = mixer_act.astype(jnp.bfloat16)
    glu_logit = jnp.dot(mixer_bf, w_glu, preferred_element_type=jnp.float32)
    mixed = (mixer_act * jax.nn.sigmoid(glu_logit)).astype(jnp.bfloat16)
    block_width = CHAN // N_TP
    branch = jnp.zeros((SEQS, D), jnp.float32)
    for shard in range(N_TP):
        partial_block = jnp.dot(mixed[:, shard * block_width:(shard + 1) * block_width], w_out[shard * block_width:(shard + 1) * block_width], preferred_element_type=jnp.float32).astype(jnp.bfloat16)
        branch = branch + lax.optimization_barrier(partial_block).astype(jnp.float32)
    after_mix = (source + branch).astype(jnp.bfloat16)
    after_float = after_mix.astype(jnp.float32)
    normed_ffn = (after_float * inverse_rms(after_float) * ffn_gain).astype(jnp.bfloat16)
    expert_ids = jnp.arange(EXPERTS, dtype=jnp.int32)
    onehot = (routes[:, :, None] == expert_ids).astype(jnp.int32)
    blocked = onehot.reshape(N_EP, SEQ_GRP * TOPK, EXPERTS)
    before = jnp.cumsum(blocked, axis=1) - blocked
    slot_index = lax.optimization_barrier(jnp.sum(before * blocked, axis=-1)).reshape(SEQS, TOPK)
    group_of_row = jnp.arange(SEQS, dtype=jnp.int32) // SEQ_GRP
    position = group_of_row[:, None] * CAP + slot_index
    columns = jnp.arange(N_EP * CAP, dtype=jnp.int32)
    hidden_width = FF_EXP // N_TP
    normed_float = normed_ffn.astype(jnp.float32)

    def apply_expert(running, expert):
        matches = (routes == expert)[:, :, None] & (position[:, :, None] == columns)
        select = jnp.any(matches, axis=1).astype(jnp.float32)
        weighting = lax.optimization_barrier(jnp.sum(jnp.where(matches, route_weights[:, :, None], 0.0), axis=1))
        expert_in = jnp.dot(select.T, normed_float, precision=highest).astype(jnp.bfloat16)
        gate_value = jnp.dot(expert_in, w_gate[expert], preferred_element_type=jnp.float32)
        up_value = jnp.dot(expert_in, w_up[expert], preferred_element_type=jnp.float32)
        hidden = (jax.nn.silu(gate_value) * up_value).astype(jnp.bfloat16)
        down_weight = w_down[expert]
        summed = jnp.zeros((N_EP * CAP, D), jnp.float32)
        for shard in range(N_TP):
            partial_block = jnp.dot(hidden[:, shard * hidden_width:(shard + 1) * hidden_width], down_weight[shard * hidden_width:(shard + 1) * hidden_width], preferred_element_type=jnp.float32).astype(jnp.bfloat16)
            summed = summed + lax.optimization_barrier(partial_block).astype(jnp.float32)
        expert_out = summed.astype(jnp.bfloat16)
        added = jnp.dot(weighting, expert_out.astype(jnp.float32), precision=highest)
        return (running + added, None)
    combined, _ = lax.scan(apply_expert, jnp.zeros((SEQS, D), jnp.float32), expert_ids)
    layer_out = (after_float + combined).astype(jnp.bfloat16)
    return (layer_out, state_next)
```

```python
import functools
import types

import jax
import jax.numpy as jnp
from jax import lax
from jax.experimental import pallas as pl
from jax.experimental.pallas import tpu as pltpu
from jax.sharding import PartitionSpec as P

TOPK = 2
epsilon = 1e-06
MESH = pl.DeviceIdType.MESH


def remote(src, dst, send_sem, recv_sem, target):
    return pltpu.make_async_remote_copy(
        src_ref=src,
        dst_ref=dst,
        send_sem=send_sem,
        recv_sem=recv_sem,
        device_id=target,
        device_id_type=MESH,
    )


def columns(place, width):
    return pl.ds(pl.multiple_of(place * width, width), width)


def flipped(place, number):
    result, bit = place, 1
    while bit <= number:
        if number & bit:
            result = result + bit - 2 * bit * lax.rem(lax.div(place, bit), 2)
        bit *= 2
    return result


def visits(experts):
    near, far = max(experts // 4, 1), experts // 2
    here = list(range(near)) + list(range(far, far + far - near))
    return here + list(range(near, far)) + list(range(far + far - near, experts))


def batches(experts):
    return [(0, experts // 2), (experts // 2, experts)]


def earlier(count):
    row = lax.broadcasted_iota(jnp.int32, (count, count), 0)
    column = lax.broadcasted_iota(jnp.int32, (count, count), 1)
    return jnp.where(row < column, 1.0, 0.0).astype(jnp.bfloat16)


def route_maps(routes_t, weights_t, experts, capacity):
    tokens = routes_t.shape[1]
    lane = lax.broadcasted_iota(jnp.int32, (experts, tokens), 0)
    picks = [jnp.where(routes_t[k : k + 1, :] == lane, 1.0, 0.0) for k in range(TOPK)]
    every = sum(picks).astype(jnp.bfloat16)
    before = jnp.dot(every, earlier(tokens), preferred_element_type=jnp.float32)
    place = lax.broadcasted_iota(jnp.int32, (experts * capacity, tokens), 0)
    sent = jnp.zeros((experts * capacity, tokens), jnp.float32)
    weighted = sent
    for k in range(TOPK):
        slot = jnp.sum(before * picks[k], axis=0, keepdims=True).astype(jnp.int32)
        match = place == routes_t[k : k + 1, :] * capacity + slot
        sent = sent + jnp.where(match, 1.0, 0.0)
        weighted = weighted + jnp.where(match, weights_t[k : k + 1, :], 0.0)
    return sent.astype(jnp.bfloat16), weighted.T


def eigen_terms(rate_ref, rotation_ref, log_step_ref):
    groups = rate_ref.shape[0]
    row = lax.broadcasted_iota(jnp.int32, (groups, groups), 0)
    column = lax.broadcasted_iota(jnp.int32, (groups, groups), 1)
    diagonal = jnp.where(row == column, log_step_ref[...], 0.0)
    step_size = jnp.exp(jnp.sum(diagonal, axis=1, keepdims=True))
    real_part, rotation = -rate_ref[...], rotation_ref[...]
    magnitude = jnp.exp(real_part * step_size)
    decay_re = magnitude * jnp.cos(rotation * step_size)
    decay_im = magnitude * jnp.sin(rotation * step_size)
    denominator = real_part * real_part + rotation * rotation
    lift_re = ((decay_re - 1.0) * real_part + decay_im * rotation) / denominator
    lift_im = (decay_im * real_part - (decay_re - 1.0) * rotation) / denominator
    return decay_re, decay_im, lift_re, lift_im


def layer_kernel(chips, names, *refs):
    r = types.SimpleNamespace(**dict(zip(names, refs)))
    ep, tp = lax.axis_index("ep"), lax.axis_index("tp")
    resid_ref = r.residual
    tokens, width = resid_ref.shape
    experts, capacity, _ = r.outb.shape
    full, units = r.gate_w.shape
    channels = r.in_w.shape[1]
    groups, group_ch, states = r.b_re.shape
    members = 2 * chips
    groups_of = batches(experts)
    core, chip = lax.rem(tp, 2), lax.div(tp, 2)
    others = [lax.rem(chip + k, chips) for k in range(1, chips)]
    origin = [lax.rem(chip + chips - 1 - j, chips) for j in range(chips - 1)]
    twin = 2 * chip + 1 - core
    partner = (ep, twin)
    peers = [lax.rem(tp + k, members) for k in range(1, members)]
    order = visits(experts)
    place_of = [flipped(ep, k) for k in order]
    mine = columns(tp, width)
    stops = others + [chip]
    last = chips - 1
    sends = []

    def load(hbm, vmem, sem):
        copy = pltpu.make_async_copy(hbm, vmem, sem)
        copy.start()
        return copy

    barrier = pltpu.get_barrier_semaphore()
    greeted = [(e, tp) for e in place_of[1:]] + [(ep, p) for p in peers]
    for target in greeted:
        pl.semaphore_signal(barrier, inc=1, device_id=target, device_id_type=MESH)
    small = [
        load(r.b_re_hbm, r.b_re, r.small_sem.at[0]),
        load(r.b_im_hbm, r.b_im, r.small_sem.at[1]),
        load(r.c_re_hbm, r.c_re, r.small_sem.at[2]),
        load(r.c_im_hbm, r.c_im, r.small_sem.at[3]),
        load(r.state_hbm, r.state, r.small_sem.at[4]),
        load(r.in_hbm, r.in_w, r.small_sem.at[5]),
        load(r.glu_hbm, r.glu_w, r.small_sem.at[6]),
        load(r.out_hbm, r.out_w, r.small_sem.at[7]),
    ]
    span_2 = 2 * states
    r.drive_w[...] = jnp.zeros_like(r.drive_w)
    r.read_w[...] = jnp.zeros_like(r.read_w)
    for g in range(groups):
        r.skip_row[:, g * group_ch : (g + 1) * group_ch] = r.skip[g : g + 1, :]
    pl.semaphore_wait(barrier, len(greeted))

    def send(*parts):
        copy = remote(*parts)
        copy.start()
        sends.append(copy)

    def arrive(block, send_sem, recv_sem):
        remote(block, block, send_sem, recv_sem, partner).wait_recv()

    own_block = r.whole.at[tp]
    for j, y in enumerate(others):
        send(resid_ref, own_block, r.wide_send.at[j], r.wide_recv.at[j], (ep, 2 * y + core))
    send(resid_ref, own_block, r.twin_send.at[0], r.twin_recv.at[0], partner)
    spread, weight = route_maps(r.routes_t[...], r.weights_t[...], experts, capacity)
    r.spread[...] = spread
    r.weight[...] = weight
    decay_re, decay_im, lift_re, lift_im = eigen_terms(r.rate, r.rotation, r.log_step)

    def project(block, place):
        x = block.astype(jnp.float32)
        square = jnp.sum(x * x, axis=1, keepdims=True)
        x = (x * r.mix_gain[:, columns(place, width)]).astype(jnp.bfloat16)
        part = jnp.dot(x, r.in_w[columns(place, width), :], preferred_element_type=jnp.float32)
        return square, part

    for copy in small[:4]:
        copy.wait()
    for g in range(groups):
        one = slice(g, g + 1)
        rows_g = slice(g * group_ch, (g + 1) * group_ch)
        left = slice(g * span_2, g * span_2 + states)
        right = slice(g * span_2 + states, (g + 1) * span_2)
        in_re, in_im = r.b_re[g], r.b_im[g]
        map_re = lift_re[one] * in_re - lift_im[one] * in_im
        map_im = lift_re[one] * in_im + lift_im[one] * in_re
        r.drive_w[rows_g, left] = map_re.astype(jnp.bfloat16)
        r.drive_w[rows_g, right] = map_im.astype(jnp.bfloat16)
        r.read_w[rows_g, left] = r.c_re[g].astype(jnp.bfloat16)
        r.read_w[rows_g, right] = (-r.c_im[g]).astype(jnp.bfloat16)
    small[4].wait()
    stride = 2 * groups
    state_rows = [
        (pl.ds(g, tokens, stride=stride), pl.ds(groups + g, tokens, stride=stride))
        for g in range(groups)
    ]
    for g, (row_re, row_im) in enumerate(state_rows):
        one = slice(g, g + 1)
        old_re, old_im = r.state[row_re, :], r.state[row_im, :]
        r.fresh[:, g * span_2 : g * span_2 + states] = (
            decay_re[one] * old_re - decay_im[one] * old_im
        )
        r.fresh[:, g * span_2 + states : (g + 1) * span_2] = (
            decay_re[one] * old_im + decay_im[one] * old_re
        )
    small[5].wait()
    square, total = project(resid_ref[...], tp)
    arrive(r.whole.at[twin], r.twin_send.at[0], r.twin_recv.at[0])
    more = project(r.whole[twin], twin)
    square, total = square + more[0], total + more[1]
    for j, y in enumerate(origin):
        place = 2 * y + core
        arrive(r.whole.at[place], r.wide_send.at[j], r.wide_recv.at[j])
        block = r.whole.at[place]
        send(block, block, r.twin_send.at[1 + j], r.twin_recv.at[1 + j], partner)
        more = project(r.whole[place], place)
        square, total = square + more[0], total + more[1]
    for j, y in enumerate(origin):
        place = 2 * y + 1 - core
        arrive(r.whole.at[place], r.twin_send.at[1 + j], r.twin_recv.at[1 + j])
        more = project(r.whole[place], place)
        square, total = square + more[0], total + more[1]
    u_in = (total * lax.rsqrt(square / full + epsilon)).astype(jnp.bfloat16)

    loads = []
    pieces = r.load_sem.shape[1]
    pairs = ((r.gate_hbm, r.gate_w), (r.up_hbm, r.up_w), (r.down_hbm, r.down_w))
    for i, (hbm, vmem) in enumerate(pairs):
        step_rows = vmem.shape[0] // pieces
        for j in range(pieces):
            span = pl.ds(j * step_rows, step_rows)
            loads.append(load(hbm.at[0, span], vmem.at[span], r.load_sem.at[i, j]))
    drive = jnp.dot(u_in, r.drive_w[...], preferred_element_type=jnp.float32)
    new = r.fresh[...] + drive
    r.fresh[...] = new
    value = lax.dot_general(
        new.astype(jnp.bfloat16),
        r.read_w[...],
        (((1,), (1,)), ((), ())),
        preferred_element_type=jnp.float32,
    )
    act = jax.nn.gelu(value + r.skip_row[...] * u_in.astype(jnp.float32))
    r.acts[tp] = act.astype(jnp.bfloat16)
    for k, p in enumerate(peers):
        send(r.acts.at[tp], r.acts.at[tp], r.act_send.at[k], r.act_recv.at[k], (ep, p))
    for g, (row_re, row_im) in enumerate(state_rows):
        r.state_out[row_re, :] = r.fresh[:, g * span_2 : g * span_2 + states]
        r.state_out[row_im, :] = r.fresh[:, g * span_2 + states : (g + 1) * span_2]

    def gate_part(place):
        return jnp.dot(
            r.acts[place], r.glu_w[columns(place, channels), :], preferred_element_type=jnp.float32
        )

    small[6].wait()
    logit = gate_part(tp)
    for k in range(members - 1):
        place = lax.rem(tp + members - 1 - k, members)
        arrive(r.acts.at[place], r.act_send.at[k], r.act_recv.at[k])
        logit = logit + gate_part(place)
    mixed = (act * jax.nn.sigmoid(logit)).astype(jnp.bfloat16)

    small[7].wait()

    def branch(place):
        return jnp.dot(
            mixed, r.out_w[:, columns(place, width)], preferred_element_type=jnp.float32
        )

    def branch_near(i, y):
        r.b_part[i] = branch(2 * y + 1 - core).astype(jnp.bfloat16)
        send(r.b_part.at[i], r.b_near.at[i], r.b_near_send.at[i], r.b_near_recv.at[i], partner)

    for i, y in enumerate(others):
        branch_near(i, y)
    for i, y in enumerate(others):
        value = branch(2 * y + core)
        arrive(r.b_near.at[i], r.b_near_send.at[i], r.b_near_recv.at[i])
        r.b_staged[i] = (value + r.b_near[i].astype(jnp.float32)).astype(jnp.bfloat16)
        target = (ep, 2 * y + core)
        send(r.b_staged.at[i], r.b_far.at[i], r.b_far_send.at[i], r.b_far_recv.at[i], target)
    branch_near(last, chip)
    value = branch(tp)
    arrive(r.b_near.at[last], r.b_near_send.at[last], r.b_near_recv.at[last])
    value = value + r.b_near[last].astype(jnp.float32)
    for i in range(last):
        arrive(r.b_far.at[i], r.b_far_send.at[i], r.b_far_recv.at[i])
        value = value + r.b_far[i].astype(jnp.float32)
    after = (resid_ref[...].astype(jnp.float32) + value).astype(jnp.bfloat16)
    r.after[...] = after
    for e in range(experts):
        picked = r.spread[e * capacity : (e + 1) * capacity, :]
        block = jnp.dot(picked, after, preferred_element_type=jnp.float32)
        r.outb[e] = block.astype(jnp.bfloat16)

    for s in range(1, experts):
        e = place_of[s]
        send(r.outb.at[e], r.rows.at[s, :, mine], r.ep_send.at[s], r.ep_recv.at[s], (e, tp))
    r.rows[0, :, mine] = r.outb[ep]

    def forward(s):
        block = r.rows.at[s, :, mine]
        if s > 0:
            arrive(block, r.ep_send.at[s], r.ep_recv.at[s])
        for j, y in enumerate(others):
            send(block, block, r.fwd_send.at[s, j], r.fwd_recv.at[s, j], (ep, 2 * y + core))
        send(block, block, r.pair_send.at[s], r.pair_recv.at[s], partner)

    def relay(s):
        for j, y in enumerate(origin):
            block = r.rows.at[s, :, columns(2 * y + core, width)]
            arrive(block, r.fwd_send.at[s, j], r.fwd_recv.at[s, j])
            send(block, block, r.relay_send.at[s, j], r.relay_recv.at[s, j], partner)

    def norm(s):
        block = r.rows.at[s, :, columns(2 * chip + 1 - core, width)]
        arrive(block, r.pair_send.at[s], r.pair_recv.at[s])
        for j, y in enumerate(origin):
            block = r.rows.at[s, :, columns(2 * y + 1 - core, width)]
            arrive(block, r.relay_send.at[s, j], r.relay_recv.at[s, j])
        total = jnp.zeros((capacity, 128), jnp.float32)
        for c in range(full // 128):
            x = r.rows[s, :, c * 128 : (c + 1) * 128].astype(jnp.float32)
            total = total + x * x
        scale = lax.rsqrt(jnp.sum(total, axis=1, keepdims=True) / full + epsilon)
        first = s * capacity
        for c in range(full // 128):
            span = slice(c * 128, (c + 1) * 128)
            x = r.rows[s, :, span].astype(jnp.float32)
            x = x * scale * r.ffn_gain[:, span]
            r.normed[first : first + capacity, span] = x.astype(jnp.bfloat16)

    tile = 512
    chunks = [(at, min(tile, units - at)) for at in range(0, units, tile)]

    def gate_up(b, start, size):
        lo, hi = groups_of[b]
        count = (hi - lo) * capacity
        x, span = r.normed[lo * capacity : hi * capacity], slice(start, start + size)
        gate = jnp.dot(x, r.gate_w[:, span], preferred_element_type=jnp.float32)
        up = jnp.dot(x, r.up_w[:, span], preferred_element_type=jnp.float32)
        value = gate * jax.nn.sigmoid(gate) * up
        r.hidden[:count, span] = value.astype(jnp.bfloat16)

    def down(b, group):
        lo, hi = groups_of[b]
        span = columns(group, width)
        value = jnp.dot(
            r.hidden[: (hi - lo) * capacity],
            r.down_w[:, span],
            preferred_element_type=jnp.float32,
        )
        r.part[lo * capacity : hi * capacity, span] = value.astype(jnp.bfloat16)

    def near_out(b, i):
        lo, hi = groups_of[b]
        span = pl.ds(lo * capacity, (hi - lo) * capacity)
        send(
            r.part.at[span, columns(2 * stops[i] + 1 - core, width)],
            r.near.at[i, span],
            r.near_send.at[b, i],
            r.near_recv.at[b, i],
            partner,
        )

    def near_in(b, i):
        lo, hi = groups_of[b]
        block = r.near.at[i, pl.ds(lo * capacity, (hi - lo) * capacity)]
        arrive(block, r.near_send.at[b, i], r.near_recv.at[b, i])

    def leaving(b):
        inside = list(range(*groups_of[b]))
        first = experts // 4
        return inside[first:] + inside[:first][::-1]

    def far_out(b, i):
        y = others[i]
        near_in(b, i)
        for s in leaving(b):
            span = slice(s * capacity, (s + 1) * capacity)
            own = r.part[span, columns(2 * y + core, width)].astype(jnp.float32)
            summed_pair = own + r.near[i, span, :].astype(jnp.float32)
            r.staged[s, i] = summed_pair.astype(jnp.bfloat16)
            send(
                r.staged.at[s, i],
                r.far.at[s, i],
                r.far_send.at[s, i],
                r.far_recv.at[s, i],
                (ep, 2 * y + core),
            )

    def give_back(s):
        span = slice(s * capacity, (s + 1) * capacity)
        total = r.part[span, mine].astype(jnp.float32)
        total = total + r.near[last, span, :].astype(jnp.float32)
        for i in range(last):
            arrive(r.far.at[s, i], r.far_send.at[s, i], r.far_recv.at[s, i])
            total = total + r.far[s, i].astype(jnp.float32)
        if s == 0:
            r.back[ep] = total.astype(jnp.bfloat16)
        else:
            r.summed[s] = total.astype(jnp.bfloat16)
            send(
                r.summed.at[s],
                r.back.at[ep],
                r.back_send.at[s],
                r.back_recv.at[s],
                (place_of[s], tp),
            )

    def run_batch(b, events):
        def step():
            for event in events.pop(0) if events else ():
                event()

        for start, size in chunks:
            gate_up(b, start, size)
            step()
        if b == 0:
            for copy in loads[2 * pieces :]:
                copy.wait()
        for i in range(chips):
            down(b, 2 * stops[i] + 1 - core)
            near_out(b, i)
        step()
        for i in range(last):
            down(b, 2 * stops[i] + core)
            far_out(b, i)
        step()
        down(b, tp)
        near_in(b, last)
        while events:
            step()

    def act_on(what, *slots):
        return [functools.partial(what, s) for s in slots]

    def spread_out(events, points):
        share = -(-len(events) // points)
        return [events[at : at + share] for at in range(0, len(events), share)]

    half, early = experts // 2, experts // 2 + experts // 4
    for s in range(early):
        forward(s)
        if 2 <= s < half + 2:
            relay(s - 2)
    for s in range(half):
        norm(s)
    for copy in loads[: 2 * pieces]:
        copy.wait()
    points = len(chunks) + 3
    events = act_on(forward, *range(early, experts)) + act_on(relay, *range(half, experts - 1))
    run_batch(0, spread_out(events, points))
    for s in range(half, early):
        norm(s)
    relay(experts - 1)
    for s in range(early, experts):
        norm(s)
    run_batch(1, spread_out(act_on(give_back, *leaving(0)), points))
    for s in leaving(1):
        give_back(s)
    for s in range(1, experts):
        landed = r.back.at[place_of[s]]
        arrive(landed, r.back_send.at[s], r.back_recv.at[s])
    weight = r.weight[...]
    coarse = weight.astype(jnp.bfloat16)
    fine = (weight - coarse.astype(jnp.float32)).astype(jnp.bfloat16)
    returned = r.back[...].reshape(experts * capacity, width)
    combined = jnp.dot(coarse, returned, preferred_element_type=jnp.float32)
    combined = combined + jnp.dot(fine, returned, preferred_element_type=jnp.float32)
    r.layer_out[...] = (r.after[...].astype(jnp.float32) + combined).astype(jnp.bfloat16)
    for copy in sends:
        copy.wait_send()


def run_layer(values, weights, experts, chips):
    residual, state = values["residual"], values["state_hbm"]
    tokens, width = residual.shape
    full, channels = weights["in_hbm"].shape
    units = weights["gate_hbm"].shape[2]
    groups, group_ch, states = weights["b_re_hbm"].shape
    capacity = 2 * tokens * TOPK // experts
    hops, members, pieces = chips - 1, 2 * chips, 4
    most = max(hi - lo for lo, hi in batches(experts)) * capacity
    dma, bf16, f32 = pltpu.SemaphoreType.DMA, jnp.bfloat16, jnp.float32
    scratch = dict(
        in_w=pltpu.VMEM((full, channels), bf16),
        state=pltpu.VMEM(state.shape, f32),
        fresh=pltpu.VMEM((tokens, 2 * groups * states), f32),
        drive_w=pltpu.VMEM((channels, 2 * groups * states), bf16),
        read_w=pltpu.VMEM((channels, 2 * groups * states), bf16),
        skip_row=pltpu.VMEM((1, channels), f32),
        b_re=pltpu.VMEM((groups, group_ch, states), f32),
        b_im=pltpu.VMEM((groups, group_ch, states), f32),
        c_re=pltpu.VMEM((groups, group_ch, states), f32),
        c_im=pltpu.VMEM((groups, group_ch, states), f32),
        glu_w=pltpu.VMEM((channels * members, channels), bf16),
        out_w=pltpu.VMEM((channels, full), bf16),
        gate_w=pltpu.VMEM((full, units), bf16),
        up_w=pltpu.VMEM((full, units), bf16),
        down_w=pltpu.VMEM((units, full), bf16),
        whole=pltpu.VMEM((members, tokens, width), bf16),
        acts=pltpu.VMEM((members, tokens, channels), bf16),
        b_part=pltpu.VMEM((chips, tokens, width), bf16),
        b_near=pltpu.VMEM((chips, tokens, width), bf16),
        b_staged=pltpu.VMEM((hops, tokens, width), bf16),
        b_far=pltpu.VMEM((hops, tokens, width), bf16),
        after=pltpu.VMEM((tokens, width), bf16),
        spread=pltpu.VMEM((experts * capacity, tokens), bf16),
        weight=pltpu.VMEM((tokens, experts * capacity), f32),
        outb=pltpu.VMEM((experts, capacity, width), bf16),
        rows=pltpu.VMEM((experts, capacity, full), bf16),
        normed=pltpu.VMEM((experts * capacity, full), bf16),
        hidden=pltpu.VMEM((most, units), bf16),
        part=pltpu.VMEM((experts * capacity, full), bf16),
        near=pltpu.VMEM((chips, experts * capacity, width), bf16),
        staged=pltpu.VMEM((experts, hops, capacity, width), bf16),
        far=pltpu.VMEM((experts, hops, capacity, width), bf16),
        summed=pltpu.VMEM((experts, capacity, width), bf16),
        back=pltpu.VMEM((experts, capacity, width), bf16),
        small_sem=dma((9,)),
        load_sem=dma((3, pieces)),
    )
    for name, shape in dict(
        wide=(hops,),
        twin=(chips,),
        act=(members - 1,),
        b_near=(chips,),
        b_far=(hops,),
        ep=(experts,),
        pair=(experts,),
        fwd=(experts, hops),
        relay=(experts, hops),
        near=(2, chips),
        far=(experts, hops),
        back=(experts,),
    ).items():
        scratch[name + "_send"] = dma(shape)
        scratch[name + "_recv"] = dma(shape)
    operands = {**values, **weights}
    vmem, hbm = pl.BlockSpec(memory_space=pltpu.VMEM), pl.BlockSpec(memory_space=pl.ANY)
    names = list(operands) + ["layer_out", "state_out"] + list(scratch)
    return pl.pallas_call(
        functools.partial(layer_kernel, chips, names),
        out_shape=(pltpu.VMEM(residual.shape, bf16), pltpu.VMEM(state.shape, f32)),
        in_specs=[hbm if name.endswith("_hbm") else vmem for name in operands],
        out_specs=(vmem, vmem),
        scratch_shapes=list(scratch.values()),
        compiler_params=pltpu.CompilerParams(
            collective_id=0, has_side_effects=True, vmem_limit_bytes=58 * 2**20
        ),
        name="layer",
    )(*operands.values())


def per_device(
    residual,
    routes,
    route_weights,
    state_prev,
    mix_gain,
    ffn_gain,
    w_in,
    decay_rate,
    rotation,
    log_step,
    in_re,
    in_im,
    read_re,
    read_im,
    skip_gain,
    w_glu,
    w_out,
    w_gate,
    w_up,
    w_down,
):
    values = dict(
        residual=residual,
        routes_t=routes.T,
        weights_t=route_weights.T,
        mix_gain=mix_gain[None, :],
        ffn_gain=ffn_gain[None, :],
        rate=decay_rate,
        rotation=rotation,
        log_step=log_step[None, :],
        skip=skip_gain,
        state_hbm=state_prev.reshape(-1, state_prev.shape[-1]),
    )
    weights = dict(
        in_hbm=w_in,
        b_re_hbm=jnp.swapaxes(in_re, 1, 2),
        b_im_hbm=jnp.swapaxes(in_im, 1, 2),
        c_re_hbm=read_re,
        c_im_hbm=read_im,
        glu_hbm=w_glu,
        out_hbm=w_out,
        gate_hbm=w_gate,
        up_hbm=w_up,
        down_hbm=w_down,
    )
    layer_out, state_next = run_layer(
        values, weights, lax.axis_size("ep"), lax.axis_size("tp") // 2
    )
    return (layer_out, state_next.reshape(state_prev.shape))


def solution(mesh):
    return jax.shard_map(
        per_device,
        mesh=mesh,
        in_specs=(
            P("ep", "tp"),
            P("ep", None),
            P("ep", None),
            P("ep", None, "tp", None),
            P(),
            P(),
            P(None, "tp"),
            P("tp", None),
            P("tp", None),
            P("tp"),
            P("tp", None, None),
            P("tp", None, None),
            P("tp", None, None),
            P("tp", None, None),
            P("tp", None),
            P(None, "tp"),
            P("tp", None),
            P("ep", None, "tp"),
            P("ep", None, "tp"),
            P("ep", "tp", None),
        ),
        out_specs=(P("ep", "tp"), P("ep", None, "tp", None)),
        check_vma=False,
    )
```

```python
import functools
import types

import jax
import jax.numpy as jnp
from jax import lax
from jax.experimental import pallas as pl
from jax.experimental.pallas import tpu as pltpu
from jax.sharding import PartitionSpec as P

TOPK = 2
TINY = [
    "routes_t",
    "weights_t",
    "mix_gain",
    "ffn_gain",
    "rate",
    "rotation",
    "log_step",
    "skip",
]
epsilon = 1e-06
MESH = pl.DeviceIdType.MESH


def remote(src, dst, send_sem, recv_sem, target):
    return pltpu.make_async_remote_copy(
        src_ref=src,
        dst_ref=dst,
        send_sem=send_sem,
        recv_sem=recv_sem,
        device_id=target,
        device_id_type=MESH,
    )


def columns(place, width):
    return pl.ds(pl.multiple_of(place * width, width), width)


def flipped(place, number):
    result, bit = place, 1
    while bit <= number:
        if number & bit:
            result = result + bit - 2 * bit * lax.rem(lax.div(place, bit), 2)
        bit *= 2
    return result


def visits(experts):
    near, far = max(experts // 4, 1), experts // 2
    here = list(range(near)) + list(range(far, far + far - near))
    return here + list(range(near, far)) + list(range(far + far - near, experts))


def batches(experts):
    return [(0, experts // 2), (experts // 2, experts)]


def earlier(count):
    row = lax.broadcasted_iota(jnp.int32, (count, count), 0)
    column = lax.broadcasted_iota(jnp.int32, (count, count), 1)
    return jnp.where(row < column, 1.0, 0.0).astype(jnp.bfloat16)


def route_maps(routes_t, weights_t, experts, capacity):
    tokens = routes_t.shape[1]
    lane = lax.broadcasted_iota(jnp.int32, (experts, tokens), 0)
    picks = [jnp.where(routes_t[k : k + 1, :] == lane, 1.0, 0.0) for k in range(TOPK)]
    every = sum(picks).astype(jnp.bfloat16)
    before = jnp.dot(every, earlier(tokens), preferred_element_type=jnp.float32)
    place = lax.broadcasted_iota(jnp.int32, (experts * capacity, tokens), 0)
    sent = jnp.zeros((experts * capacity, tokens), jnp.float32)
    weighted = sent
    for k in range(TOPK):
        slot = jnp.sum(before * picks[k], axis=0, keepdims=True).astype(jnp.int32)
        match = place == routes_t[k : k + 1, :] * capacity + slot
        sent = sent + jnp.where(match, 1.0, 0.0)
        weighted = weighted + jnp.where(match, weights_t[k : k + 1, :], 0.0)
    return sent.astype(jnp.bfloat16), weighted.T


def eigen_terms(rate_ref, rotation_ref, log_step_ref):
    groups = rate_ref.shape[0]
    row = lax.broadcasted_iota(jnp.int32, (groups, groups), 0)
    column = lax.broadcasted_iota(jnp.int32, (groups, groups), 1)
    diagonal = jnp.where(row == column, log_step_ref[...], 0.0)
    step_size = jnp.exp(jnp.sum(diagonal, axis=1, keepdims=True))
    real_part, rotation = -rate_ref[...], rotation_ref[...]
    magnitude = jnp.exp(real_part * step_size)
    decay_re = magnitude * jnp.cos(rotation * step_size)
    decay_im = magnitude * jnp.sin(rotation * step_size)
    denominator = real_part * real_part + rotation * rotation
    lift_re = ((decay_re - 1.0) * real_part + decay_im * rotation) / denominator
    lift_im = (decay_im * real_part - (decay_re - 1.0) * rotation) / denominator
    return decay_re, decay_im, lift_re, lift_im


def layer_kernel(chips, names, *refs):
    r = types.SimpleNamespace(**dict(zip(names, refs)))
    ep, tp = lax.axis_index("ep"), lax.axis_index("tp")
    resid_ref = r.residual
    tokens, width = resid_ref.shape
    experts, capacity, _ = r.outb.shape
    full, units = r.gate_w.shape
    channels = r.in_w.shape[1]
    groups, group_ch, states = r.b_re.shape
    members = 2 * chips
    groups_of = batches(experts)
    core, chip = lax.rem(tp, 2), lax.div(tp, 2)
    others = [lax.rem(chip + k, chips) for k in range(1, chips)]
    origin = [lax.rem(chip + chips - 1 - j, chips) for j in range(chips - 1)]
    twin = 2 * chip + 1 - core
    partner = (ep, twin)
    peers = [lax.rem(tp + k, members) for k in range(1, members)]
    order = visits(experts)
    place_of = [flipped(ep, k) for k in order]
    mine = columns(tp, width)
    stops = others + [chip]
    last = chips - 1
    sends = []

    def load(hbm, vmem, sem):
        copy = pltpu.make_async_copy(hbm, vmem, sem)
        copy.start()
        return copy

    barrier = pltpu.get_barrier_semaphore()
    greeted = [(e, tp) for e in place_of[1:]] + [(ep, p) for p in peers]
    for target in greeted:
        pl.semaphore_signal(barrier, inc=1, device_id=target, device_id_type=MESH)
    lead = load(r.residual_hbm, r.residual, r.lead_sem.at[0])
    tiny = [
        load(getattr(r, name + "_hbm"), getattr(r, name), r.lead_sem.at[1 + at])
        for at, name in enumerate(TINY)
    ]
    small = [
        load(r.b_re_hbm, r.b_re, r.small_sem.at[0]),
        load(r.b_im_hbm, r.b_im, r.small_sem.at[1]),
        load(r.c_re_hbm, r.c_re, r.small_sem.at[2]),
        load(r.c_im_hbm, r.c_im, r.small_sem.at[3]),
        load(r.state_hbm, r.state, r.small_sem.at[4]),
        load(r.in_hbm, r.in_w, r.small_sem.at[5]),
        load(r.glu_hbm, r.glu_w, r.small_sem.at[6]),
        load(r.out_hbm, r.out_w, r.small_sem.at[7]),
    ]
    span_2 = 2 * states
    r.drive_w[...] = jnp.zeros_like(r.drive_w)
    r.read_w[...] = jnp.zeros_like(r.read_w)
    pl.semaphore_wait(barrier, len(greeted))

    def send(*parts):
        copy = remote(*parts)
        copy.start()
        sends.append(copy)

    def arrive(block, send_sem, recv_sem):
        remote(block, block, send_sem, recv_sem, partner).wait_recv()

    lead.wait()
    own_block = r.whole.at[tp]
    for j, y in enumerate(others):
        send(resid_ref, own_block, r.wide_send.at[j], r.wide_recv.at[j], (ep, 2 * y + core))
    send(resid_ref, own_block, r.twin_send.at[0], r.twin_recv.at[0], partner)
    for copy in tiny:
        copy.wait()
    spread, weight = route_maps(r.routes_t[...], r.weights_t[...], experts, capacity)
    r.spread[...] = spread
    r.weight[...] = weight
    decay_re, decay_im, lift_re, lift_im = eigen_terms(r.rate, r.rotation, r.log_step)

    def project(block, place):
        x = block.astype(jnp.float32)
        square = jnp.sum(x * x, axis=1, keepdims=True)
        x = (x * r.mix_gain[:, columns(place, width)]).astype(jnp.bfloat16)
        part = jnp.dot(x, r.in_w[columns(place, width), :], preferred_element_type=jnp.float32)
        return square, part

    for copy in small[:4]:
        copy.wait()
    for g in range(groups):
        r.skip_row[:, g * group_ch : (g + 1) * group_ch] = r.skip[g : g + 1, :]
    for g in range(groups):
        one = slice(g, g + 1)
        rows_g = slice(g * group_ch, (g + 1) * group_ch)
        left = slice(g * span_2, g * span_2 + states)
        right = slice(g * span_2 + states, (g + 1) * span_2)
        in_re, in_im = r.b_re[g], r.b_im[g]
        map_re = lift_re[one] * in_re - lift_im[one] * in_im
        map_im = lift_re[one] * in_im + lift_im[one] * in_re
        r.drive_w[rows_g, left] = map_re.astype(jnp.bfloat16)
        r.drive_w[rows_g, right] = map_im.astype(jnp.bfloat16)
        r.read_w[rows_g, left] = r.c_re[g].astype(jnp.bfloat16)
        r.read_w[rows_g, right] = (-r.c_im[g]).astype(jnp.bfloat16)
    small[4].wait()
    stride = 2 * groups
    state_rows = [
        (pl.ds(g, tokens, stride=stride), pl.ds(groups + g, tokens, stride=stride))
        for g in range(groups)
    ]
    for g, (row_re, row_im) in enumerate(state_rows):
        one = slice(g, g + 1)
        old_re, old_im = r.state[row_re, :], r.state[row_im, :]
        r.fresh[:, g * span_2 : g * span_2 + states] = (
            decay_re[one] * old_re - decay_im[one] * old_im
        )
        r.fresh[:, g * span_2 + states : (g + 1) * span_2] = (
            decay_re[one] * old_im + decay_im[one] * old_re
        )
    small[5].wait()
    square, total = project(resid_ref[...], tp)
    arrive(r.whole.at[twin], r.twin_send.at[0], r.twin_recv.at[0])
    more = project(r.whole[twin], twin)
    square, total = square + more[0], total + more[1]
    for j, y in enumerate(origin):
        place = 2 * y + core
        arrive(r.whole.at[place], r.wide_send.at[j], r.wide_recv.at[j])
        block = r.whole.at[place]
        send(block, block, r.twin_send.at[1 + j], r.twin_recv.at[1 + j], partner)
        more = project(r.whole[place], place)
        square, total = square + more[0], total + more[1]
    for j, y in enumerate(origin):
        place = 2 * y + 1 - core
        arrive(r.whole.at[place], r.twin_send.at[1 + j], r.twin_recv.at[1 + j])
        more = project(r.whole[place], place)
        square, total = square + more[0], total + more[1]
    u_in = (total * lax.rsqrt(square / full + epsilon)).astype(jnp.bfloat16)

    loads = []
    pieces = r.load_sem.shape[1]
    pairs = ((r.gate_hbm, r.gate_w), (r.up_hbm, r.up_w), (r.down_hbm, r.down_w))
    for i, (hbm, vmem) in enumerate(pairs):
        step_rows = vmem.shape[0] // pieces
        for j in range(pieces):
            span = pl.ds(j * step_rows, step_rows)
            loads.append(load(hbm.at[0, span], vmem.at[span], r.load_sem.at[i, j]))
    drive = jnp.dot(u_in, r.drive_w[...], preferred_element_type=jnp.float32)
    new = r.fresh[...] + drive
    r.fresh[...] = new
    value = lax.dot_general(
        new.astype(jnp.bfloat16),
        r.read_w[...],
        (((1,), (1,)), ((), ())),
        preferred_element_type=jnp.float32,
    )
    act = jax.nn.gelu(value + r.skip_row[...] * u_in.astype(jnp.float32))
    r.acts[tp] = act.astype(jnp.bfloat16)
    for k, p in enumerate(peers):
        send(r.acts.at[tp], r.acts.at[tp], r.act_send.at[k], r.act_recv.at[k], (ep, p))
    for g, (row_re, row_im) in enumerate(state_rows):
        r.state_out[row_re, :] = r.fresh[:, g * span_2 : g * span_2 + states]
        r.state_out[row_im, :] = r.fresh[:, g * span_2 + states : (g + 1) * span_2]

    def gate_part(place):
        return jnp.dot(
            r.acts[place], r.glu_w[columns(place, channels), :], preferred_element_type=jnp.float32
        )

    small[6].wait()
    logit = gate_part(tp)
    for k in range(members - 1):
        place = lax.rem(tp + members - 1 - k, members)
        arrive(r.acts.at[place], r.act_send.at[k], r.act_recv.at[k])
        logit = logit + gate_part(place)
    mixed = (act * jax.nn.sigmoid(logit)).astype(jnp.bfloat16)

    small[7].wait()

    cut = width // 2
    cuts = [slice(0, cut), slice(cut, width)]

    def branch(place, q):
        span = pl.ds(pl.multiple_of(place * width + q * cut, cut), cut)
        return jnp.dot(mixed, r.out_w[:, span], preferred_element_type=jnp.float32)

    def branch_near(i, y):
        for q, span in enumerate(cuts):
            r.b_part[i, :, span] = branch(2 * y + 1 - core, q).astype(jnp.bfloat16)
            send(
                r.b_part.at[i, :, span],
                r.b_near.at[i, :, span],
                r.b_near_send.at[i, q],
                r.b_near_recv.at[i, q],
                partner,
            )

    def branch_sum(i, y, q):
        value = branch(2 * y + core, q)
        block = r.b_near.at[i, :, cuts[q]]
        arrive(block, r.b_near_send.at[i, q], r.b_near_recv.at[i, q])
        return value + r.b_near[i, :, cuts[q]].astype(jnp.float32)

    for i, y in enumerate(others):
        branch_near(i, y)
    for i, y in enumerate(others):
        for q, span in enumerate(cuts):
            r.b_staged[i, :, span] = branch_sum(i, y, q).astype(jnp.bfloat16)
            send(
                r.b_staged.at[i, :, span],
                r.b_far.at[i, :, span],
                r.b_far_send.at[i, q],
                r.b_far_recv.at[i, q],
                (ep, 2 * y + core),
            )
    branch_near(last, chip)
    for q, span in enumerate(cuts):
        r.after_sum[:, span] = resid_ref[:, span].astype(jnp.float32) + branch_sum(last, chip, q)
    value = r.after_sum[...]
    for i in range(last):
        for q, span in enumerate(cuts):
            block = r.b_far.at[i, :, span]
            arrive(block, r.b_far_send.at[i, q], r.b_far_recv.at[i, q])
        value = value + r.b_far[i].astype(jnp.float32)
    after = value.astype(jnp.bfloat16)
    r.after[...] = after
    for e in range(experts):
        picked = r.spread[e * capacity : (e + 1) * capacity, :]
        block = jnp.dot(picked, after, preferred_element_type=jnp.float32)
        r.outb[e] = block.astype(jnp.bfloat16)

    for s in range(1, experts):
        e = place_of[s]
        send(r.outb.at[e], r.rows.at[s, :, mine], r.ep_send.at[s], r.ep_recv.at[s], (e, tp))
    r.rows[0, :, mine] = r.outb[ep]

    def forward(s):
        block = r.rows.at[s, :, mine]
        if s > 0:
            arrive(block, r.ep_send.at[s], r.ep_recv.at[s])
        for j, y in enumerate(others):
            send(block, block, r.fwd_send.at[s, j], r.fwd_recv.at[s, j], (ep, 2 * y + core))
        send(block, block, r.pair_send.at[s], r.pair_recv.at[s], partner)

    def relay(s):
        for j, y in enumerate(origin):
            block = r.rows.at[s, :, columns(2 * y + core, width)]
            arrive(block, r.fwd_send.at[s, j], r.fwd_recv.at[s, j])
            send(block, block, r.relay_send.at[s, j], r.relay_recv.at[s, j], partner)

    def norm(s):
        block = r.rows.at[s, :, columns(2 * chip + 1 - core, width)]
        arrive(block, r.pair_send.at[s], r.pair_recv.at[s])
        for j, y in enumerate(origin):
            block = r.rows.at[s, :, columns(2 * y + 1 - core, width)]
            arrive(block, r.relay_send.at[s, j], r.relay_recv.at[s, j])
        total = jnp.zeros((capacity, 128), jnp.float32)
        for c in range(full // 128):
            x = r.rows[s, :, c * 128 : (c + 1) * 128].astype(jnp.float32)
            total = total + x * x
        scale = lax.rsqrt(jnp.sum(total, axis=1, keepdims=True) / full + epsilon)
        first = s * capacity
        for c in range(full // 128):
            span = slice(c * 128, (c + 1) * 128)
            x = r.rows[s, :, span].astype(jnp.float32)
            x = x * scale * r.ffn_gain[:, span]
            r.normed[first : first + capacity, span] = x.astype(jnp.bfloat16)

    tile = 256
    chunks = [(at, min(tile, units - at)) for at in range(0, units, tile)]

    def gate_up(b, start, size):
        lo, hi = groups_of[b]
        count = (hi - lo) * capacity
        x, span = r.normed[lo * capacity : hi * capacity], slice(start, start + size)
        gate = jnp.dot(x, r.gate_w[:, span], preferred_element_type=jnp.float32)
        up = jnp.dot(x, r.up_w[:, span], preferred_element_type=jnp.float32)
        value = gate * jax.nn.sigmoid(gate) * up
        r.hidden[:count, span] = value.astype(jnp.bfloat16)

    def down(b, group):
        lo, hi = groups_of[b]
        span = columns(group, width)
        value = jnp.dot(
            r.hidden[: (hi - lo) * capacity],
            r.down_w[:, span],
            preferred_element_type=jnp.float32,
        )
        r.part[lo * capacity : hi * capacity, span] = value.astype(jnp.bfloat16)

    def near_out(b, i):
        lo, hi = groups_of[b]
        span = pl.ds(lo * capacity, (hi - lo) * capacity)
        send(
            r.part.at[span, columns(2 * stops[i] + 1 - core, width)],
            r.near.at[i, span],
            r.near_send.at[b, i],
            r.near_recv.at[b, i],
            partner,
        )

    def near_in(b, i):
        lo, hi = groups_of[b]
        block = r.near.at[i, pl.ds(lo * capacity, (hi - lo) * capacity)]
        arrive(block, r.near_send.at[b, i], r.near_recv.at[b, i])

    def leaving(b):
        inside = list(range(*groups_of[b]))
        first = experts // 4
        return inside[first:] + inside[:first][::-1]

    def far_out(b, i):
        y = others[i]
        near_in(b, i)
        for s in leaving(b):
            span = slice(s * capacity, (s + 1) * capacity)
            own = r.part[span, columns(2 * y + core, width)].astype(jnp.float32)
            summed_pair = own + r.near[i, span, :].astype(jnp.float32)
            r.staged[s, i] = summed_pair.astype(jnp.bfloat16)
            send(
                r.staged.at[s, i],
                r.far.at[s, i],
                r.far_send.at[s, i],
                r.far_recv.at[s, i],
                (ep, 2 * y + core),
            )

    def give_back(s):
        span = slice(s * capacity, (s + 1) * capacity)
        total = r.part[span, mine].astype(jnp.float32)
        total = total + r.near[last, span, :].astype(jnp.float32)
        for i in range(last):
            arrive(r.far.at[s, i], r.far_send.at[s, i], r.far_recv.at[s, i])
            total = total + r.far[s, i].astype(jnp.float32)
        if s == 0:
            r.back[ep] = total.astype(jnp.bfloat16)
        else:
            r.summed[s] = total.astype(jnp.bfloat16)
            send(
                r.summed.at[s],
                r.back.at[ep],
                r.back_send.at[s],
                r.back_recv.at[s],
                (place_of[s], tp),
            )

    def run_batch(b, events):
        def step():
            for event in events.pop(0) if events else ():
                event()

        for at, (start, size) in enumerate(chunks):
            gate_up(b, start, size)
            if at in pauses[b]:
                step()
        if b == 0:
            for copy in loads[2 * pieces :]:
                copy.wait()
        for i in range(chips):
            down(b, 2 * stops[i] + 1 - core)
            near_out(b, i)
        step()
        for i in range(last):
            down(b, 2 * stops[i] + core)
            far_out(b, i)
        step()
        down(b, tp)
        near_in(b, last)
        while events:
            step()

    def act_on(what, *slots):
        return [functools.partial(what, s) for s in slots]

    def spread_out(events, points):
        share = -(-len(events) // points)
        return [events[at : at + share] for at in range(0, len(events), share)]

    half, early = experts // 2, experts // 2 + experts // 4
    for s in range(early):
        forward(s)
        if 2 <= s < half + 2:
            relay(s - 2)
    for s in range(half):
        norm(s)
    for copy in loads[: 2 * pieces]:
        copy.wait()
    pauses = ({len(chunks) // 3}, {len(chunks) - 1})
    events = spread_out(act_on(relay, *range(half, experts - 1)), 3)
    run_batch(0, [act_on(forward, *range(early, experts))] + events)
    relay(experts - 1)
    for s in range(half, experts):
        norm(s)
    run_batch(1, [[]] + spread_out(act_on(give_back, *leaving(0)), 2))
    for s in leaving(1):
        give_back(s)
    for s in range(1, experts):
        landed = r.back.at[place_of[s]]
        arrive(landed, r.back_send.at[s], r.back_recv.at[s])
    weight = r.weight[...]
    coarse = weight.astype(jnp.bfloat16)
    fine = (weight - coarse.astype(jnp.float32)).astype(jnp.bfloat16)
    returned = r.back[...].reshape(experts * capacity, width)
    combined = jnp.dot(coarse, returned, preferred_element_type=jnp.float32)
    combined = combined + jnp.dot(fine, returned, preferred_element_type=jnp.float32)
    r.layer_out[...] = (r.after[...].astype(jnp.float32) + combined).astype(jnp.bfloat16)
    for copy in sends:
        copy.wait_send()


def run_layer(values, weights, experts, chips):
    values = {name if name == "state_hbm" else name + "_hbm": a for name, a in values.items()}
    residual, state = values["residual_hbm"], values["state_hbm"]
    tokens, width = residual.shape
    full, channels = weights["in_hbm"].shape
    units = weights["gate_hbm"].shape[2]
    groups, group_ch, states = weights["b_re_hbm"].shape
    capacity = 2 * tokens * TOPK // experts
    hops, members, pieces = chips - 1, 2 * chips, 4
    most = max(hi - lo for lo, hi in batches(experts)) * capacity
    dma, bf16, f32 = pltpu.SemaphoreType.DMA, jnp.bfloat16, jnp.float32
    scratch = {
        name: pltpu.VMEM(values[name + "_hbm"].shape, values[name + "_hbm"].dtype)
        for name in ["residual"] + TINY
    }
    scratch.update(
        in_w=pltpu.VMEM((full, channels), bf16),
        state=pltpu.VMEM(state.shape, f32),
        fresh=pltpu.VMEM((tokens, 2 * groups * states), f32),
        drive_w=pltpu.VMEM((channels, 2 * groups * states), bf16),
        read_w=pltpu.VMEM((channels, 2 * groups * states), bf16),
        skip_row=pltpu.VMEM((1, channels), f32),
        b_re=pltpu.VMEM((groups, group_ch, states), f32),
        b_im=pltpu.VMEM((groups, group_ch, states), f32),
        c_re=pltpu.VMEM((groups, group_ch, states), f32),
        c_im=pltpu.VMEM((groups, group_ch, states), f32),
        glu_w=pltpu.VMEM((channels * members, channels), bf16),
        out_w=pltpu.VMEM((channels, full), bf16),
        gate_w=pltpu.VMEM((full, units), bf16),
        up_w=pltpu.VMEM((full, units), bf16),
        down_w=pltpu.VMEM((units, full), bf16),
        whole=pltpu.VMEM((members, tokens, width), bf16),
        acts=pltpu.VMEM((members, tokens, channels), bf16),
        b_part=pltpu.VMEM((chips, tokens, width), bf16),
        b_near=pltpu.VMEM((chips, tokens, width), bf16),
        b_staged=pltpu.VMEM((hops, tokens, width), bf16),
        b_far=pltpu.VMEM((hops, tokens, width), bf16),
        after_sum=pltpu.VMEM((tokens, width), f32),
        after=pltpu.VMEM((tokens, width), bf16),
        spread=pltpu.VMEM((experts * capacity, tokens), bf16),
        weight=pltpu.VMEM((tokens, experts * capacity), f32),
        outb=pltpu.VMEM((experts, capacity, width), bf16),
        rows=pltpu.VMEM((experts, capacity, full), bf16),
        normed=pltpu.VMEM((experts * capacity, full), bf16),
        hidden=pltpu.VMEM((most, units), bf16),
        part=pltpu.VMEM((experts * capacity, full), bf16),
        near=pltpu.VMEM((chips, experts * capacity, width), bf16),
        staged=pltpu.VMEM((experts, hops, capacity, width), bf16),
        far=pltpu.VMEM((experts, hops, capacity, width), bf16),
        summed=pltpu.VMEM((experts, capacity, width), bf16),
        back=pltpu.VMEM((experts, capacity, width), bf16),
        lead_sem=dma((1 + len(TINY),)),
        small_sem=dma((8,)),
        load_sem=dma((3, pieces)),
    )
    for name, shape in dict(
        wide=(hops,),
        twin=(chips,),
        act=(members - 1,),
        b_near=(chips, 2),
        b_far=(hops, 2),
        ep=(experts,),
        pair=(experts,),
        fwd=(experts, hops),
        relay=(experts, hops),
        near=(2, chips),
        far=(experts, hops),
        back=(experts,),
    ).items():
        scratch[name + "_send"] = dma(shape)
        scratch[name + "_recv"] = dma(shape)
    operands = {**values, **weights}
    vmem, hbm = pl.BlockSpec(memory_space=pltpu.VMEM), pl.BlockSpec(memory_space=pl.ANY)
    names = list(operands) + ["layer_out", "state_out"] + list(scratch)
    return pl.pallas_call(
        functools.partial(layer_kernel, chips, names),
        out_shape=(pltpu.VMEM(residual.shape, bf16), pltpu.VMEM(state.shape, f32)),
        in_specs=[hbm if name.endswith("_hbm") else vmem for name in operands],
        out_specs=(vmem, vmem),
        scratch_shapes=list(scratch.values()),
        compiler_params=pltpu.CompilerParams(
            collective_id=0, has_side_effects=True, vmem_limit_bytes=58 * 2**20
        ),
        name="layer",
    )(*operands.values())


def store_kernel(count, *refs):
    sems = refs[-1]
    copies = [
        pltpu.make_async_copy(refs[i], refs[count + i], sems.at[i]) for i in range(count)
    ]
    for copy in copies:
        copy.start()
    for copy in copies:
        copy.wait()


def store(*arrays):
    vmem, hbm = pl.BlockSpec(memory_space=pltpu.VMEM), pl.BlockSpec(memory_space=pl.ANY)
    held = [pltpu.with_memory_space_constraint(a, pltpu.VMEM) for a in arrays]
    return pl.pallas_call(
        functools.partial(store_kernel, len(arrays)),
        out_shape=tuple(jax.ShapeDtypeStruct(a.shape, a.dtype) for a in arrays),
        in_specs=[vmem] * len(arrays),
        out_specs=(hbm,) * len(arrays),
        scratch_shapes=[pltpu.SemaphoreType.DMA((len(arrays),))],
        name="store",
    )(*held)


def per_device(
    residual,
    routes,
    route_weights,
    state_prev,
    mix_gain,
    ffn_gain,
    w_in,
    decay_rate,
    rotation,
    log_step,
    in_re,
    in_im,
    read_re,
    read_im,
    skip_gain,
    w_glu,
    w_out,
    w_gate,
    w_up,
    w_down,
):
    values = dict(
        residual=residual,
        routes_t=routes.T,
        weights_t=route_weights.T,
        mix_gain=mix_gain[None, :],
        ffn_gain=ffn_gain[None, :],
        rate=decay_rate,
        rotation=rotation,
        log_step=log_step[None, :],
        skip=skip_gain,
        state_hbm=state_prev.reshape(-1, state_prev.shape[-1]),
    )
    weights = dict(
        in_hbm=w_in,
        b_re_hbm=jnp.swapaxes(in_re, 1, 2),
        b_im_hbm=jnp.swapaxes(in_im, 1, 2),
        c_re_hbm=read_re,
        c_im_hbm=read_im,
        glu_hbm=w_glu,
        out_hbm=w_out,
        gate_hbm=w_gate,
        up_hbm=w_up,
        down_hbm=w_down,
    )
    layer_out, state_next = run_layer(
        values, weights, lax.axis_size("ep"), lax.axis_size("tp") // 2
    )
    layer_out, state_next = store(layer_out, state_next)
    return (layer_out, state_next.reshape(state_prev.shape))


def solution(mesh):
    return jax.shard_map(
        per_device,
        mesh=mesh,
        in_specs=(
            P("ep", "tp"),
            P("ep", None),
            P("ep", None),
            P("ep", None, "tp", None),
            P(),
            P(),
            P(None, "tp"),
            P("tp", None),
            P("tp", None),
            P("tp"),
            P("tp", None, None),
            P("tp", None, None),
            P("tp", None, None),
            P("tp", None, None),
            P("tp", None),
            P(None, "tp"),
            P("tp", None),
            P("ep", None, "tp"),
            P("ep", None, "tp"),
            P("ep", "tp", None),
        ),
        out_specs=(P("ep", "tp"), P("ep", None, "tp", None)),
        check_vma=False,
    )
```
